128 devices in a mesh: ep: 32 (over z, y, core), tp: 4 (over x).
Axes of the slice: x: 4, y: 4, z: 4, core: 2. Of those that a mesh axis runs over, the one named last changes fastest.
Arguments:
- pool_in: bfloat16 [32768, 1024], P(('ep', 'tp')), may hold values from -6 to 6
- pool_map: bfloat16 [4, 256, 256], replicated, may hold values from -0.375 to 0.375
- pool_scale: float32 [1024], replicated, may hold values from 0.1 to 1.9
- w_out: bfloat16 [1024, 2048], replicated, may hold values from -0.1875 to 0.1875
- mix_gain: float32 [2048], replicated, may hold values from 0.1 to 1.9
- ffn_in: bfloat16 [16384, 2048], P(('ep', 'tp')), may hold values from -6 to 6
- ffn_gain: float32 [2048], replicated, may hold values from 0.1 to 1.9
- routes: int32 [16384, 2], P(('ep', 'tp')), may hold values from 0 to 31, all different within a row; in each aligned block of 128 rows (0 to 127, 128 to 255, ...) at most 10 rows name the same one
- route_weight: float32 [16384, 2], P(('ep', 'tp')), may hold values from 0.1 to 1
- w_gate: bfloat16 [32, 2048, 5632], P('ep', None, 'tp'), may hold values from -0.125 to 0.125
- w_up: bfloat16 [32, 2048, 5632], P('ep', None, 'tp'), may hold values from -0.125 to 0.125
- w_down: bfloat16 [32, 5632, 2048], P('ep', 'tp'), may hold values from -0.078125 to 0.078125
- out_gain: float32 [2048], replicated, may hold values from 0.1 to 1.9
Outputs:
- mixer_out: bfloat16 [32768, 2048], P(('ep', 'tp'))
- moe_out: bfloat16 [16384, 2048], P(('ep', 'tp'))
The draws below stay inside these ranges and needn't reach their ends.
Inputs may be any that keep to these rules, and one draw needn't show every extreme that they name: `routes`: each row names two different experts. Among the 128 rows of one device (aligned blocks of rows), no expert is named more than 10 times, and in every draw some expert is named exactly 10 times by the rows of some device.
All inputs are finite; a program needn't handle non-finite values.
Results may differ from the reference program's by a relative error of at most 0.012.
Values may be sent and summed in bfloat16 or wider, within the bound.
No kernel may reach another device: no remote copies, remote signals or barrier semaphores. Data moves between devices by JAX's collectives and lax.ppermute only.
A program may use at most 128 MiB of HBM per device.

```python
import math
import jax
import jax.numpy as jnp
import numpy as np
from jax import lax

D = 2048
GROUPS = 4
GC = 256
FFE = 5632
EXPERTS = 32
TOK2_DEV = 128
TOK1 = 32768
TOK2 = 16384
CAP = 10
N_EP = 32
N_TP = 4


def block_levels(rng, dims, shards, smallest, top_value):
    def one(dim, blocks):
        draws = jax.random.uniform(jax.random.fold_in(jax.random.fold_in(rng, 6), dim), (blocks,), jnp.float32, smallest / len(shards), top_value / len(shards))
        return jnp.repeat(jnp.exp(draws), dims[dim] // blocks).reshape((-1,) + (1,) * (len(dims) - dim - 1))

    level = one(*shards[0])
    for cut in shards[1:]:
        level = level * one(*cut)
    return level


def assign_block(own_key, own, number, rows, count, top, limit, skew):
    order = jax.random.permutation(own_key, count)
    packed, usual = load_shares(count, rows * top, limit, skew, True), load_shares(count, rows * top, limit, skew, False)
    places = jnp.arange(count)

    def named(lengths, turn):
        used = int((lengths > 0).sum())
        fixed = max(1, used // 4)
        passed = fixed + (places - fixed + turn * (used - fixed)) % max(1, count - fixed)
        return jnp.zeros((count,), jnp.int32).at[order[jnp.where(places < fixed, places, passed)]].set(jnp.asarray(lengths, jnp.int32))

    lengths = jnp.where(number % 4 == 0, named(packed, number // 4), named(usual, number - number // 4 - 1))
    mixed = jax.random.permutation(jax.random.fold_in(own, 3), count)
    giver, sink = mixed[0:count // 2 * 2:2], mixed[1:count // 2 * 2:2]
    slack = jnp.minimum(lengths[giver] - 1, limit - lengths[sink]) // 2
    slack = jnp.where((giver == order[0]) | (sink == order[0]) | (lengths[sink] == 0), 0, jnp.maximum(slack, 0))
    passed = jax.random.randint(jax.random.fold_in(own, 4), (count // 2,), 0, 1 << 20) % (slack + 1)
    lengths = lengths.at[giver].add(-passed).at[sink].add(passed)
    items = jnp.searchsorted(jnp.cumsum(lengths), jnp.arange(rows * top), side="right").astype(jnp.int32)
    grid = items.reshape(top, rows).T
    grid = grid[jax.random.permutation(jax.random.fold_in(own, 1), rows)]
    turn = jax.random.randint(jax.random.fold_in(own, 2), (rows, 1), 0, top)
    return jnp.take_along_axis(grid, (jnp.arange(top)[None, :] + turn) % top, axis=1)


def load_shares(count, total, bound, skew, full):
    loads = [(1 << 20) // math.isqrt(grade ** skew) + 1 for grade in range(1, count + 1)]
    largest = bound if full else min(bound, max(-(-total // count), total * loads[0] // sum(loads)))
    least = 1 if total - largest >= count - 1 else 0
    holding, rest = [largest] + [least] * (count - 1), total - largest - least * (count - 1)
    while rest > 0:
        candidates = [i for i in range(1, count) if holding[i] < largest] or [i for i in range(1, count) if holding[i] < bound]
        mass, left = sum([loads[i] for i in candidates]), rest
        for i in candidates:
            addition = min(bound - holding[i], max(1, left * loads[i] // mass), rest)
            holding[i] = holding[i] + addition
            rest = rest - addition
    return np.array(holding)


def gaussian(rng, shape, deviation, limit, split=(), held_as=jnp.bfloat16):
    result = jax.random.normal(rng, shape, jnp.float32) * deviation
    if len(split) > 0:
        result = block_levels(rng, shape, split, -0.22, 0.18) * result
    return jnp.clip(result, min=-limit, max=limit).astype(held_as)


def setup_inputs(seed: int = 0) -> dict:
    streams_of = jax.random.split(jax.random.key(seed), 14)
    pool_in = gaussian(streams_of[0], (TOK1, GROUPS * GC), 1.0, 6.0, ((0, 128),))
    pool_map = gaussian(streams_of[1], (GROUPS, GC, GC), GC ** -0.5, 0.375)
    pool_scale = jnp.clip(1.0 + 0.18 * jax.random.normal(streams_of[2], (GROUPS * GC,), jnp.float32), 0.1, 1.9)
    w_out = gaussian(streams_of[3], (GROUPS * GC, D), (GROUPS * GC) ** -0.5, 0.1875)
    mix_gain = jnp.clip(1.0 + 0.18 * jax.random.normal(streams_of[4], (D,), jnp.float32), 0.1, 1.9)
    ffn_in = gaussian(streams_of[5], (TOK2, D), 1.0, 6.0, ((0, 128),))
    ffn_gain = jnp.clip(1.0 + 0.18 * jax.random.normal(streams_of[6], (D,), jnp.float32), 0.1, 1.9)
    routes_keys = jax.random.split(jax.random.fold_in(streams_of[7], 1), TOK2 // TOK2_DEV)
    routes_turns = jax.random.permutation(jax.random.fold_in(streams_of[7], 3), TOK2 // TOK2_DEV)
    routes = jax.vmap(lambda own, number: assign_block(jax.random.fold_in(streams_of[7], 2), own, number, TOK2_DEV, EXPERTS, 2, CAP, 1))(routes_keys, routes_turns).reshape((TOK2, 2))
    route_weight = jnp.clip(0.1 + 0.9 * jax.random.uniform(streams_of[8], (TOK2, 2), jnp.float32) ** block_levels(streams_of[8], (TOK2, 2), ((0, 128),), -0.2, 0.2), 0.1, 1.0)
    w_gate = gaussian(streams_of[9], (EXPERTS, D, FFE), D ** -0.5, 0.125, ((0, 32), (2, 4)))
    w_up = gaussian(streams_of[10], (EXPERTS, D, FFE), D ** -0.5, 0.125, ((0, 32), (2, 4)))
    w_down = gaussian(streams_of[11], (EXPERTS, FFE, D), FFE ** -0.5, 0.078125, ((0, 32), (1, 4)))
    out_gain = jnp.clip(1.0 + 0.18 * jax.random.normal(streams_of[12], (D,), jnp.float32), 0.1, 1.9)
    return {"pool_in": pool_in, "pool_map": pool_map, "pool_scale": pool_scale, "w_out": w_out, "mix_gain": mix_gain, "ffn_in": ffn_in, "ffn_gain": ffn_gain, "routes": routes, "route_weight": route_weight, "w_gate": w_gate, "w_up": w_up, "w_down": w_down, "out_gain": out_gain}


epsilon = 1e-06

def rounded(values):
    return lax.optimization_barrier(values.astype(jnp.bfloat16)).astype(jnp.float32)

def normalize(values, gain):
    return values * lax.rsqrt(lax.optimization_barrier(jnp.mean(values * values, axis=-1, keepdims=True)) + epsilon) * gain

def reference(pool_in, pool_map, pool_scale, w_out, mix_gain, ffn_in, ffn_gain, routes, route_weight, w_gate, w_up, w_down, out_gain):
    signal = pool_in.astype(jnp.float32)
    seq_len = signal.shape[0]
    padded = jnp.pad(signal, ((15, 0), (0, 0)))
    position = jnp.arange(seq_len, dtype=jnp.float32)
    group_maps = []
    for step_index in range(GROUPS):
        window = 2 ** (step_index + 1)
        columns = padded[:, step_index * GC:(step_index + 1) * GC]
        window_sum = columns[15:15 + seq_len]
        for offset in range(1, window):
            window_sum = window_sum + columns[15 - offset:15 - offset + seq_len]
        divisor = jnp.minimum(position + 1.0, float(window))[:, None]
        contrast = rounded(window_sum / divisor - signal[:, step_index * GC:(step_index + 1) * GC])
        group_maps.append(jnp.dot(contrast, pool_map[step_index].astype(jnp.float32), preferred_element_type=jnp.float32))
    pooled = rounded(jnp.concatenate(group_maps, axis=1) * pool_scale)
    projected = jnp.dot(pooled, w_out.astype(jnp.float32), preferred_element_type=jnp.float32)
    mixer_out = normalize(projected, mix_gain).astype(jnp.bfloat16)
    normed = normalize(ffn_in.astype(jnp.float32), ffn_gain).astype(jnp.bfloat16)
    chosen = routes.reshape(-1).astype(jnp.int32)
    route_count = chosen.shape[0]
    one_hot = (chosen[:, None] == jnp.arange(EXPERTS, dtype=jnp.int32)[None, :]).astype(jnp.int32)
    slot_rank = lax.optimization_barrier(jnp.sum((jnp.cumsum(one_hot, axis=0, dtype=jnp.int32) - 1) * one_hot, axis=1)).astype(jnp.int32)
    slot_count = N_EP * N_TP * CAP
    slot_table = jnp.zeros((EXPERTS, slot_count), jnp.int32).at[chosen, slot_rank].set((jnp.arange(route_count, dtype=jnp.int32) // 2).astype(jnp.int32))
    shard_len = FFE // N_TP

    def expert(operands):
        gate_w, up_w, down_w, tok_index = operands
        tok_rows = normed[tok_index].astype(jnp.float32)
        gate_pre = jnp.dot(tok_rows, gate_w.astype(jnp.float32), preferred_element_type=jnp.float32)
        up_pre = jnp.dot(tok_rows, up_w.astype(jnp.float32), preferred_element_type=jnp.float32)
        hidden = rounded(jax.nn.silu(gate_pre) * up_pre)
        total = jnp.zeros((tok_rows.shape[0], D), jnp.float32)
        for shard in range(N_TP):
            total = total + rounded(jnp.dot(hidden[:, shard * shard_len:(shard + 1) * shard_len], down_w[shard * shard_len:(shard + 1) * shard_len].astype(jnp.float32), preferred_element_type=jnp.float32))
        return total.astype(jnp.bfloat16)
    outputs = lax.map(expert, (w_gate, w_up, w_down, slot_table))
    picked = outputs[chosen, slot_rank].astype(jnp.float32).reshape(route_count // 2, 2, D)
    combined = lax.optimization_barrier(jnp.sum(picked * route_weight[:, :, None], axis=1))
    moe_out = normalize(combined, out_gain).astype(jnp.bfloat16)
    return (mixer_out, moe_out)
```

```python
import functools

import jax
import jax.numpy as jnp
from jax import lax
from jax.experimental import pallas as pl
from jax.experimental.pallas import tpu as pltpu
from jax.sharding import PartitionSpec as P

epsilon = 1e-06
bf16 = jnp.bfloat16
f32 = jnp.float32

CHUNKS = ((4,), (4, 2))


def layout(features):
    chunks, first = [], 0
    for sizes in CHUNKS:
        parts, lane = [], 0
        for size in sizes:
            parts.append((size, first, lane, size * features // 8))
            first += size
            lane += size * features // 8
        chunks.append((tuple(parts), lane))
    return chunks


def dot(a, b):
    return jnp.dot(a, b, preferred_element_type=f32)


def dot_t(a, b):
    return lax.dot_general(a, b, (((0,), (0,)), ((), ())), preferred_element_type=f32)


def iota(shape, dim):
    return lax.broadcasted_iota(jnp.int32, shape, dim)


def normalize(values, gain):
    return values * lax.rsqrt(jnp.mean(values * values, axis=-1, keepdims=True) + epsilon) * gain


def ranks(experts, routes_ref):
    tokens = routes_ref.shape[1]
    first, second = routes_ref[0:1, :], routes_ref[1:2, :]
    names = iota((experts, tokens), 0)
    hot = [(names == chosen).astype(f32) for chosen in (first, second)]
    before = (iota((tokens, tokens), 0) < iota((tokens, tokens), 1)).astype(bf16)
    ahead = [dot(h.astype(bf16), before) for h in hot]
    ahead[1] = ahead[1] + jnp.sum(hot[0], axis=1, keepdims=True)
    rank = [jnp.sum(h * a, axis=0, keepdims=True).astype(jnp.int32) for h, a in zip(hot, ahead)]
    return (first, second), rank


def places(experts, tokens, chosen, rank, part, j):
    size, first, _, _ = part
    rows = iota((experts * 8, tokens), 0)
    found = []
    for e, r in zip(chosen, rank):
        inside = (r >= first) & (r < first + size)
        found.append(rows == jnp.where(inside, e * 8 + j * size + r - first, -1))
    return found


def pack_kernel(chunks, routes_ref, rows_ref, gain_ref, *wire_refs):
    experts = wire_refs[0].shape[0] // 8
    tokens = routes_ref.shape[1]
    normed = normalize(rows_ref[...].astype(f32), gain_ref[...]).astype(bf16)
    chosen, rank = ranks(experts, routes_ref)
    for (parts, _), wire_ref in zip(chunks, wire_refs):
        for part in parts:
            _, _, lane, width = part
            total = None
            for j in range(normed.shape[1] // width):
                found = places(experts, tokens, chosen, rank, part, j)
                taken = dot((found[0] | found[1]).astype(f32).astype(bf16), normed[:, j * width : (j + 1) * width])
                total = taken if total is None else total + taken
            wire_ref[:, lane : lane + width] = total.astype(bf16)


def combine_kernel(chunks, routes_ref, weight_ref, gain_ref, *refs):
    wire_refs, out_ref, total = refs[:-2], refs[-2], refs[-1]
    experts = wire_refs[0].shape[0] // 8
    tokens = routes_ref.shape[1]
    features = out_ref.shape[1]
    chosen, rank = ranks(experts, routes_ref)
    weights = (weight_ref[0:1, :], weight_ref[1:2, :])
    total[...] = jnp.zeros_like(total)
    for (parts, _), wire_ref in zip(chunks, wire_refs):
        for part in parts:
            _, _, lane, width = part
            for j in range(features // width):
                found = places(experts, tokens, chosen, rank, part, j)
                scale = jnp.where(found[0], weights[0], 0.0) + jnp.where(found[1], weights[1], 0.0)
                high = scale.astype(bf16)
                low = (scale - high.astype(f32)).astype(bf16)
                held = wire_ref[:, lane : lane + width]
                total[:, j * width : (j + 1) * width] += dot_t(high, held) + dot_t(low, held)
    out_ref[...] = normalize(total[...], gain_ref[...]).astype(out_ref.dtype)


def expert_kernel(parts, count, *refs):
    wires, (gate_ref, up_ref, down_ref) = refs[:count], refs[count : count + 3]
    outs = refs[count + 3 : 2 * count + 3]
    rows_ref, hidden_ref, result_ref, gate_buf, up_buf, rest_buf, down_buf, gate_sem, up_sem, rest_sem, down_sem = refs[
        2 * count + 3 :
    ]
    features, hidden = gate_ref.shape
    block = 256
    full = hidden // block
    rest = hidden - full * block
    wide = 512

    def gate_copy(i):
        cols = pl.ds(pl.multiple_of(i * block, block), block)
        return pltpu.make_async_copy(gate_ref.at[:, cols], gate_buf.at[:, cols], gate_sem.at[i])

    def up_copy(i):
        cols = pl.ds(pl.multiple_of(i * block, block), block)
        return pltpu.make_async_copy(up_ref.at[:, cols], up_buf.at[:, cols], up_sem.at[i])

    def down_copy(i):
        cols = pl.ds(pl.multiple_of(i * wide, wide), wide)
        return pltpu.make_async_copy(down_ref.at[:, cols], down_buf.at[:, cols], down_sem.at[i])

    tails = [
        pltpu.make_async_copy(ref.at[:, pl.ds(full * block, rest)], rest_buf.at[:, pl.ds(k * rest, rest)], rest_sem.at[k])
        for k, ref in enumerate((gate_ref, up_ref))
    ]
    for i in range(full):
        gate_copy(i).start()
        up_copy(i).start()
    for tail in tails:
        tail.start()
    for i in range(features // wide):
        down_copy(i).start()

    places_of = []
    base = 0
    for wire in wires:
        experts = wire.shape[0] // 8
        for size, _, lane, width in parts:
            length = experts * size
            places_of.append((wire, base, length, size, lane, width))
            base += length

    def picking(length, size, j, across):
        shape = (length * 8 // size, length) if across else (length, length * 8 // size)
        row, place = iota(shape, 1 if across else 0), iota(shape, 0 if across else 1)
        return (place == row // size * 8 + j * size + row % size).astype(f32).astype(bf16)

    for wire, start, length, size, lane, width in places_of:
        for j in range(8 // size):
            held = wire[:, lane : lane + width]
            if size < 8:
                held = dot(picking(length, size, j, False), held).astype(bf16)
            rows_ref[start : start + length, j * width : (j + 1) * width] = held

    def first(i, carry):
        gate_copy(i).wait()
        up_copy(i).wait()
        cols = pl.ds(pl.multiple_of(i * block, block), block)
        gate = dot(rows_ref[...], gate_buf[:, cols])
        up = dot(rows_ref[...], up_buf[:, cols])
        hidden_ref[:, cols] = (gate / (1.0 + jnp.exp(-gate)) * up).astype(bf16)
        return carry

    lax.fori_loop(0, full, first, 0)
    for tail in tails:
        tail.wait()
    both = dot(rows_ref[...], rest_buf[...])
    gate, up = both[:, :rest], both[:, rest:]
    hidden_ref[:, full * block :] = (gate / (1.0 + jnp.exp(-gate)) * up).astype(bf16)

    def second(i, carry):
        down_copy(i).wait()
        cols = pl.ds(pl.multiple_of(i * wide, wide), wide)
        result_ref[:, cols] = dot(hidden_ref[...], down_buf[:, cols]).astype(bf16)
        return carry

    lax.fori_loop(0, features // wide, second, 0)

    for (wire, start, length, size, lane, width), out in zip(
        places_of, [out for out in outs for _ in parts]
    ):
        total = None
        for j in range(8 // size):
            held = result_ref[start : start + length, j * width : (j + 1) * width]
            if size < 8:
                held = dot(picking(length, size, j, True), held)
            total = held if total is None else total + held
        out[:, lane : lane + width] = total.astype(bf16)


def vmem(count):
    return [pl.BlockSpec(memory_space=pltpu.VMEM)] * count


def expert_block(parts, wires, w_gate, w_up, w_down):
    features, hidden = w_gate.shape
    slots = sum(part[0] for part in parts)
    rows = sum(wire.shape[0] // 8 * slots for wire in wires)
    rest = hidden % 256
    return pl.pallas_call(
        functools.partial(expert_kernel, parts, len(wires)),
        out_shape=[jax.ShapeDtypeStruct(wire.shape, bf16) for wire in wires],
        in_specs=vmem(len(wires)) + [pl.BlockSpec(memory_space=pl.ANY)] * 3,
        out_specs=vmem(len(wires)),
        scratch_shapes=[
            pltpu.VMEM((rows, features), bf16),
            pltpu.VMEM((rows, hidden), bf16),
            pltpu.VMEM((rows, features), bf16),
            pltpu.VMEM((features, hidden - rest), bf16),
            pltpu.VMEM((features, hidden - rest), bf16),
            pltpu.VMEM((features, 2 * rest), bf16),
            pltpu.VMEM((hidden, features), bf16),
            pltpu.SemaphoreType.DMA((hidden // 256,)),
            pltpu.SemaphoreType.DMA((hidden // 256,)),
            pltpu.SemaphoreType.DMA((2,)),
            pltpu.SemaphoreType.DMA((features // 512,)),
        ],
        compiler_params=pltpu.CompilerParams(vmem_limit_bytes=44 * 2**20),
        cost_estimate=pl.CostEstimate(
            flops=6 * rows * features * hidden,
            bytes_accessed=6 * features * hidden + 4 * rows * features,
            transcendentals=rows * hidden,
        ),
        name="experts",
    )(*wires, w_gate, w_up, w_down)


def ring(step):
    count = lax.axis_size("tp")
    return [(t, (t + step) % count) for t in range(count)]


def rightward(value):
    return lax.ppermute(value, "tp", ring(1))


def leftward(value):
    return lax.ppermute(value, "tp", ring(-1))


def added(*values):
    return sum(value.astype(f32) for value in values).astype(bf16)


def exchange(wire):
    experts = lax.axis_size("ep")
    blocks = wire.reshape(experts, 8, wire.shape[1])
    return lax.all_to_all(blocks, "ep", split_axis=0, concat_axis=0, tiled=True).reshape(wire.shape)


def routed_experts(ffn_in, ffn_gain, routes, route_weight, w_gate, w_up, w_down, out_gain):
    tokens, features = ffn_in.shape
    experts = lax.axis_size("ep")
    chunks = layout(features)
    routes_t, weight_t = routes.T, route_weight.T
    wires = pl.pallas_call(
        functools.partial(pack_kernel, chunks),
        out_shape=[jax.ShapeDtypeStruct((experts * 8, width), bf16) for _, width in chunks],
        in_specs=vmem(3),
        out_specs=vmem(len(chunks)),
        compiler_params=pltpu.CompilerParams(vmem_limit_bytes=24 * 2**20),
        cost_estimate=pl.CostEstimate(flops=2**30, bytes_accessed=2**21, transcendentals=0),
        name="pack",
    )(routes_t, ffn_in, ffn_gain[None])
    returned = []
    for (parts, _), wire in zip(chunks, wires):
        own = exchange(wire)
        half = own.shape[0] // 2
        weights = (w_gate[0], w_up[0], w_down[0])
        left, right = rightward(own), leftward(own)
        far_a, far_b = rightward(left[:half]), leftward(right[half:])
        own, left, right = expert_block(parts, [own, left, right], *weights)
        far_a, far_b = expert_block(parts, [far_a, far_b], *weights)
        far_a, far_b = leftward(far_a), rightward(far_b)
        left = jnp.concatenate([added(left[:half], far_a), left[half:]])
        right = jnp.concatenate([right[:half], added(right[half:], far_b)])
        returned.append(exchange(added(own, leftward(left), rightward(right))))
    return pl.pallas_call(
        functools.partial(combine_kernel, chunks),
        out_shape=jax.ShapeDtypeStruct(ffn_in.shape, bf16),
        in_specs=vmem(3 + len(chunks)),
        out_specs=pl.BlockSpec(memory_space=pltpu.VMEM),
        scratch_shapes=[pltpu.VMEM((tokens, features), f32)],
        compiler_params=pltpu.CompilerParams(vmem_limit_bytes=24 * 2**20),
        cost_estimate=pl.CostEstimate(flops=2**30, bytes_accessed=2**21, transcendentals=0),
        name="combine",
    )(routes_t, weight_t, out_gain[None], *returned)


def pool_mixer(pool_in, pool_map, pool_scale, w_out, mix_gain):
    own_rows, channels = pool_in.shape
    group_count, group_width = pool_map.shape[0], pool_map.shape[1]
    axes = ("ep", "tp")
    count = lax.axis_size(axes)
    previous = lax.ppermute(pool_in[own_rows - 16 :], axes, [(d, d + 1) for d in range(count - 1)])
    running = jnp.concatenate([previous, pool_in], axis=0).astype(f32)
    window_parts = []
    stride = 1
    for step_index in range(group_count):
        running = running[stride:] + running[:-stride]
        stride = stride * 2
        window_parts.append(running[-own_rows:, step_index * group_width : (step_index + 1) * group_width])
    windows = jnp.concatenate(window_parts, axis=1)
    offset = lax.axis_index(axes) * own_rows
    position = (offset + jnp.arange(own_rows, dtype=jnp.int32)).astype(f32)
    reaches = (2 ** (1 + jnp.arange(channels, dtype=jnp.int32) // group_width)).astype(f32)
    counts = jnp.minimum(position[:, None] + 1.0, reaches[None, :])
    contrast = (windows / counts - pool_in.astype(f32)).astype(bf16)
    mapped = jnp.einsum(
        "rgc,gcd->rgd",
        contrast.reshape(own_rows, group_count, group_width),
        pool_map,
        preferred_element_type=f32,
    ).reshape(own_rows, channels)
    pooled = (mapped * pool_scale).astype(bf16)
    projected = jnp.dot(pooled, w_out, preferred_element_type=f32)
    return normalize(projected, mix_gain).astype(bf16)


def shards(
    pool_in,
    pool_map,
    pool_scale,
    w_out,
    mix_gain,
    ffn_in,
    ffn_gain,
    routes,
    route_weight,
    w_gate,
    w_up,
    w_down,
    out_gain,
):
    mixer_out = pool_mixer(pool_in, pool_map, pool_scale, w_out, mix_gain)
    moe_out = routed_experts(ffn_in, ffn_gain, routes, route_weight, w_gate, w_up, w_down, out_gain)
    return (mixer_out, moe_out)


def solution(mesh):
    return jax.shard_map(
        shards,
        mesh=mesh,
        in_specs=(
            P(("ep", "tp"), None),
            P(),
            P(),
            P(),
            P(),
            P(("ep", "tp"), None),
            P(),
            P(("ep", "tp"), None),
            P(("ep", "tp"), None),
            P("ep", None, "tp"),
            P("ep", None, "tp"),
            P("ep", "tp", None),
            P(),
        ),
        out_specs=(P(("ep", "tp"), None), P(("ep", "tp"), None)),
        check_vma=False,
    )
```

```python
import functools

import jax
import jax.numpy as jnp
from jax import lax
from jax.experimental import pallas as pl
from jax.experimental.pallas import tpu as pltpu
from jax.sharding import PartitionSpec as P


epsilon = 1e-06
bf16 = jnp.bfloat16
f32 = jnp.float32

CHUNKS = ((8, 2),)
STEPS = 4


def layout(features):
    chunks, first = [], 0
    for sizes in CHUNKS:
        parts, lane = [], 0
        for size in sizes:
            parts.append((size, first, lane, size * features // 8))
            first += size
            lane += size * features // 8
        chunks.append((tuple(parts), lane))
    return chunks


def dot(a, b):
    return jnp.dot(a, b, preferred_element_type=f32)


def dot_t(a, b):
    return lax.dot_general(a, b, (((0,), (0,)), ((), ())), preferred_element_type=f32)


def iota(shape, dim):
    return lax.broadcasted_iota(jnp.int32, shape, dim)


def normalize(values, gain):
    return values * lax.rsqrt(jnp.mean(values * values, axis=-1, keepdims=True) + epsilon) * gain


def ranks(experts, routes_ref):
    tokens = routes_ref.shape[1]
    first, second = routes_ref[0:1, :], routes_ref[1:2, :]
    names = iota((experts, tokens), 0)
    hot = [(names == chosen).astype(f32) for chosen in (first, second)]
    before = (iota((tokens, tokens), 0) < iota((tokens, tokens), 1)).astype(bf16)
    ahead = [dot(h.astype(bf16), before) for h in hot]
    ahead[1] = ahead[1] + jnp.sum(hot[0], axis=1, keepdims=True)
    rank = [jnp.sum(h * a, axis=0, keepdims=True).astype(jnp.int32) for h, a in zip(hot, ahead)]
    return (first, second), rank


def places(experts, tokens, chosen, rank, part, j):
    size, first, _, _ = part
    rows = iota((experts * 8, tokens), 0)
    found = []
    for e, r in zip(chosen, rank):
        inside = (r >= first) & (r < first + size)
        found.append(rows == jnp.where(inside, e * 8 + j * size + r - first, -1))
    return found


def pack_kernel(chunks, routes_ref, rows_ref, gain_ref, *wire_refs):
    experts = wire_refs[0].shape[0] // 8
    tokens = routes_ref.shape[1]
    normed = normalize(rows_ref[...].astype(f32), gain_ref[...]).astype(bf16)
    chosen, rank = ranks(experts, routes_ref)
    for (parts, _), wire_ref in zip(chunks, wire_refs):
        for part in parts:
            _, _, lane, width = part
            total = None
            for j in range(normed.shape[1] // width):
                found = places(experts, tokens, chosen, rank, part, j)
                taken = dot((found[0] | found[1]).astype(f32).astype(bf16), normed[:, j * width : (j + 1) * width])
                total = taken if total is None else total + taken
            wire_ref[:, lane : lane + width] = total.astype(bf16)


def combine_kernel(chunks, routes_ref, weight_ref, gain_ref, *refs):
    wire_refs, out_ref, total = refs[:-2], refs[-2], refs[-1]
    experts = wire_refs[0].shape[0] // 8
    tokens = routes_ref.shape[1]
    features = out_ref.shape[1]
    chosen, rank = ranks(experts, routes_ref)
    weights = (weight_ref[0:1, :], weight_ref[1:2, :])
    total[...] = jnp.zeros_like(total)
    for (parts, _), wire_ref in zip(chunks, wire_refs):
        for part in parts:
            _, _, lane, width = part
            for j in range(features // width):
                found = places(experts, tokens, chosen, rank, part, j)
                scale = jnp.where(found[0], weights[0], 0.0) + jnp.where(found[1], weights[1], 0.0)
                high = scale.astype(bf16)
                low = (scale - high.astype(f32)).astype(bf16)
                held = wire_ref[:, lane : lane + width]
                total[:, j * width : (j + 1) * width] += dot_t(high, held) + dot_t(low, held)
    out_ref[...] = normalize(total[...], gain_ref[...]).astype(out_ref.dtype)


def expert_kernel(parts, count, *refs):
    wires, (gate_ref, up_ref, down_ref) = refs[:count], refs[count : count + 3]
    outs = refs[count + 3 : 2 * count + 3]
    rows_ref, hidden_ref, result_ref, gate_sum, up_sum, gate_buf, up_buf, down_buf, sems = refs[2 * count + 3 :]
    features, hidden = gate_ref.shape
    deep = features // STEPS
    wide = 512

    def fetch(source, target, length, k, sem):
        rows = pl.ds(k * length, length)
        return pltpu.make_async_copy(source.at[rows], target.at[rows], sem)

    gate_copies = [fetch(gate_ref, gate_buf, deep, k, sems.at[k]) for k in range(STEPS)]
    up_copies = [fetch(up_ref, up_buf, deep, k, sems.at[STEPS + k]) for k in range(STEPS)]
    down_copies = [fetch(down_ref, down_buf, hidden // 2, k, sems.at[2 * STEPS + k]) for k in range(2)]
    for gate_copy, up_copy in zip(gate_copies, up_copies):
        gate_copy.start()
        up_copy.start()
    for down_copy in down_copies:
        down_copy.start()

    places_of = []
    base = 0
    for wire in wires:
        experts = wire.shape[0] // 8
        for size, _, lane, width in parts:
            length = experts * size
            places_of.append((wire, base, length, size, lane, width))
            base += length

    def picking(length, size, j, across):
        shape = (length * 8 // size, length) if across else (length, length * 8 // size)
        row, place = iota(shape, 1 if across else 0), iota(shape, 0 if across else 1)
        return (place == row // size * 8 + j * size + row % size).astype(f32).astype(bf16)

    for wire, start, length, size, lane, width in places_of:
        for j in range(8 // size):
            held = wire[:, lane : lane + width]
            if size < 8:
                held = dot(picking(length, size, j, False), held).astype(bf16)
            rows_ref[start : start + length, j * width : (j + 1) * width] = held

    for k in range(STEPS):
        gate_copies[k].wait()
        up_copies[k].wait()
        held = rows_ref[:, k * deep : (k + 1) * deep]
        for start in range(0, hidden, wide):
            cols = slice(start, min(start + wide, hidden))
            gate = dot(held, gate_buf[k * deep : (k + 1) * deep, cols])
            up = dot(held, up_buf[k * deep : (k + 1) * deep, cols])
            if k > 0:
                gate, up = gate_sum[:, cols] + gate, up_sum[:, cols] + up
            if k < STEPS - 1:
                gate_sum[:, cols], up_sum[:, cols] = gate, up
            else:
                hidden_ref[:, cols] = (gate / (1.0 + jnp.exp(-gate)) * up).astype(bf16)
    for down_copy in down_copies:
        down_copy.wait()

    def second(i, carry):
        cols = pl.ds(pl.multiple_of(i * wide, wide), wide)
        result_ref[:, cols] = dot(hidden_ref[...], down_buf[:, cols]).astype(bf16)
        return carry

    lax.fori_loop(0, features // wide, second, 0)

    for (wire, start, length, size, lane, width), out in zip(
        places_of, [out for out in outs for _ in parts]
    ):
        total = None
        for j in range(8 // size):
            held = result_ref[start : start + length, j * width : (j + 1) * width]
            if size < 8:
                held = dot(picking(length, size, j, True), held)
            total = held if total is None else total + held
        out[:, lane : lane + width] = total.astype(bf16)


def vmem(count):
    return [pl.BlockSpec(memory_space=pltpu.VMEM)] * count


def expert_block(parts, wires, w_gate, w_up, w_down):
    features, hidden = w_gate.shape
    slots = sum(part[0] for part in parts)
    rows = sum(wire.shape[0] // 8 * slots for wire in wires)
    return pl.pallas_call(
        functools.partial(expert_kernel, parts, len(wires)),
        out_shape=[jax.ShapeDtypeStruct(wire.shape, bf16) for wire in wires],
        in_specs=vmem(len(wires)) + [pl.BlockSpec(memory_space=pl.ANY)] * 3,
        out_specs=vmem(len(wires)),
        scratch_shapes=[
            pltpu.VMEM((rows, features), bf16),
            pltpu.VMEM((rows, hidden), bf16),
            pltpu.VMEM((rows, features), bf16),
            pltpu.VMEM((rows, hidden), f32),
            pltpu.VMEM((rows, hidden), f32),
            pltpu.VMEM((features, hidden), bf16),
            pltpu.VMEM((features, hidden), bf16),
            pltpu.VMEM((hidden, features), bf16),
            pltpu.SemaphoreType.DMA((2 * STEPS + 2,)),
        ],
        compiler_params=pltpu.CompilerParams(vmem_limit_bytes=54 * 2**20),
        cost_estimate=pl.CostEstimate(
            flops=6 * rows * features * hidden,
            bytes_accessed=6 * features * hidden + 4 * rows * features,
            transcendentals=rows * hidden,
        ),
        name="experts",
    )(*wires, w_gate, w_up, w_down)


def ring(step):
    count = lax.axis_size("tp")
    return [(t, (t + step) % count) for t in range(count)]


def rightward(value):
    return lax.ppermute(value, "tp", ring(1))


def leftward(value):
    return lax.ppermute(value, "tp", ring(-1))


def added(*values):
    return sum(value.astype(f32) for value in values).astype(bf16)


def exchange(wire):
    experts = lax.axis_size("ep")
    blocks = wire.reshape(experts, 8, wire.shape[1])
    return lax.all_to_all(blocks, "ep", split_axis=0, concat_axis=0, tiled=True).reshape(wire.shape)


def routed_experts(ffn_in, ffn_gain, routes, route_weight, w_gate, w_up, w_down, out_gain):
    tokens, features = ffn_in.shape
    experts = lax.axis_size("ep")
    chunks = layout(features)
    routes_t, weight_t = routes.T, route_weight.T
    wires = pl.pallas_call(
        functools.partial(pack_kernel, chunks),
        out_shape=[jax.ShapeDtypeStruct((experts * 8, width), bf16) for _, width in chunks],
        in_specs=vmem(3),
        out_specs=vmem(len(chunks)),
        compiler_params=pltpu.CompilerParams(vmem_limit_bytes=8 * 2**20),
        cost_estimate=pl.CostEstimate(flops=2**30, bytes_accessed=2**21, transcendentals=0),
        name="pack",
    )(routes_t, ffn_in, ffn_gain[None])
    ((parts, _),) = chunks
    (wire,) = wires
    compute = functools.partial(expert_block, parts, w_gate=w_gate[0], w_up=w_up[0], w_down=w_down[0])
    own = exchange(wire)
    half = own.shape[0] // 2
    left_a, right_b = rightward(own[:half]), leftward(own[half:])
    left_b, right_a = rightward(own[half:]), leftward(own[:half])
    far_a, far_b = rightward(left_a), leftward(right_b)
    (own,) = compute([own])
    left_a, right_b = compute([left_a, right_b])
    left_b, right_a = compute([left_b, right_a])
    far_a, far_b = compute([far_a, far_b])
    from_right_b, from_left_a = leftward(left_b), rightward(right_a)
    far_a, far_b = leftward(far_a), rightward(far_b)
    from_right_a, from_left_b = leftward(added(left_a, far_a)), rightward(added(right_b, far_b))
    total = jnp.concatenate([added(own[:half], from_left_a, from_right_a), added(own[half:], from_right_b, from_left_b)])
    returned = [exchange(total)]
    return pl.pallas_call(
        functools.partial(combine_kernel, chunks),
        out_shape=jax.ShapeDtypeStruct(ffn_in.shape, bf16),
        in_specs=vmem(3 + len(chunks)),
        out_specs=pl.BlockSpec(memory_space=pltpu.VMEM),
        scratch_shapes=[pltpu.VMEM((tokens, features), f32)],
        compiler_params=pltpu.CompilerParams(vmem_limit_bytes=8 * 2**20),
        cost_estimate=pl.CostEstimate(flops=2**30, bytes_accessed=2**21, transcendentals=0),
        name="combine",
    )(routes_t, weight_t, out_gain[None], *returned)


def pool_mixer(pool_in, pool_map, pool_scale, w_out, mix_gain):
    own_rows, channels = pool_in.shape
    group_count, group_width = pool_map.shape[0], pool_map.shape[1]
    axes = ("ep", "tp")
    count = lax.axis_size(axes)
    previous = lax.ppermute(pool_in[own_rows - 16 :], axes, [(d, d + 1) for d in range(count - 1)])
    running = jnp.concatenate([previous, pool_in], axis=0).astype(f32)
    window_parts = []
    stride = 1
    for step_index in range(group_count):
        running = running[stride:] + running[:-stride]
        stride = stride * 2
        window_parts.append(running[-own_rows:, step_index * group_width : (step_index + 1) * group_width])
    windows = jnp.concatenate(window_parts, axis=1)
    offset = lax.axis_index(axes) * own_rows
    position = (offset + jnp.arange(own_rows, dtype=jnp.int32)).astype(f32)
    reaches = (2 ** (1 + jnp.arange(channels, dtype=jnp.int32) // group_width)).astype(f32)
    counts = jnp.minimum(position[:, None] + 1.0, reaches[None, :])
    contrast = (windows / counts - pool_in.astype(f32)).astype(bf16)
    mapped = jnp.einsum(
        "rgc,gcd->rgd",
        contrast.reshape(own_rows, group_count, group_width),
        pool_map,
        preferred_element_type=f32,
    ).reshape(own_rows, channels)
    pooled = (mapped * pool_scale).astype(bf16)
    projected = jnp.dot(pooled, w_out, preferred_element_type=f32)
    return normalize(projected, mix_gain).astype(bf16)


def shards(
    pool_in,
    pool_map,
    pool_scale,
    w_out,
    mix_gain,
    ffn_in,
    ffn_gain,
    routes,
    route_weight,
    w_gate,
    w_up,
    w_down,
    out_gain,
):
    mixer_out = pool_mixer(pool_in, pool_map, pool_scale, w_out, mix_gain)
    moe_out = routed_experts(ffn_in, ffn_gain, routes, route_weight, w_gate, w_up, w_down, out_gain)
    return (mixer_out, moe_out)


def solution(mesh):
    return jax.shard_map(
        shards,
        mesh=mesh,
        in_specs=(
            P(("ep", "tp"), None),
            P(),
            P(),
            P(),
            P(),
            P(("ep", "tp"), None),
            P(),
            P(("ep", "tp"), None),
            P(("ep", "tp"), None),
            P("ep", None, "tp"),
            P("ep", None, "tp"),
            P("ep", "tp", None),
            P(),
        ),
        out_specs=(P(("ep", "tp"), None), P(("ep", "tp"), None)),
        check_vma=False,
    )
```

```python
import functools

import jax
import jax.numpy as jnp
from jax import lax
from jax.experimental import pallas as pl
from jax.experimental.pallas import tpu as pltpu
from jax.sharding import PartitionSpec as P


epsilon = 1e-06
bf16 = jnp.bfloat16
f32 = jnp.float32

CHUNKS = ((8, 2),)
LIMIT = 14


def layout(features):
    chunks, first = [], 0
    for sizes in CHUNKS:
        parts, lane = [], 0
        for size in sizes:
            parts.append((size, first, lane, size * features // 8))
            first += size
            lane += size * features // 8
        chunks.append((tuple(parts), lane))
    return chunks


def dot(a, b):
    return jnp.dot(a, b, preferred_element_type=f32)


def dot_t(a, b):
    return lax.dot_general(a, b, (((0,), (0,)), ((), ())), preferred_element_type=f32)


def iota(shape, dim):
    return lax.broadcasted_iota(jnp.int32, shape, dim)


def normalize(values, gain):
    return values * lax.rsqrt(jnp.mean(values * values, axis=-1, keepdims=True) + epsilon) * gain


def ranks(experts, routes_ref):
    tokens = routes_ref.shape[1]
    first, second = routes_ref[0:1, :], routes_ref[1:2, :]
    names = iota((experts, tokens), 0)
    hot = [(names == chosen).astype(f32) for chosen in (first, second)]
    before = (iota((tokens, tokens), 0) < iota((tokens, tokens), 1)).astype(bf16)
    ahead = [dot(h.astype(bf16), before) for h in hot]
    ahead[1] = ahead[1] + jnp.sum(hot[0], axis=1, keepdims=True)
    rank = [jnp.sum(h * a, axis=0, keepdims=True).astype(jnp.int32) for h, a in zip(hot, ahead)]
    return (first, second), rank


def places(experts, tokens, chosen, rank, part, j):
    size, first, _, _ = part
    rows = iota((experts * 8, tokens), 0)
    found = []
    for e, r in zip(chosen, rank):
        inside = (r >= first) & (r < first + size)
        found.append(rows == jnp.where(inside, e * 8 + j * size + r - first, -1))
    return found


def pack_kernel(chunks, routes_ref, rows_ref, gain_ref, *wire_refs):
    experts = wire_refs[0].shape[0] // 8
    tokens = routes_ref.shape[1]
    normed = normalize(rows_ref[...].astype(f32), gain_ref[...]).astype(bf16)
    chosen, rank = ranks(experts, routes_ref)
    for (parts, _), wire_ref in zip(chunks, wire_refs):
        for part in parts:
            _, _, lane, width = part
            total = None
            for j in range(normed.shape[1] // width):
                found = places(experts, tokens, chosen, rank, part, j)
                taken = dot((found[0] | found[1]).astype(f32).astype(bf16), normed[:, j * width : (j + 1) * width])
                total = taken if total is None else total + taken
            wire_ref[:, lane : lane + width] = total.astype(bf16)


def combine_kernel(chunks, routes_ref, weight_ref, gain_ref, *refs):
    wire_refs, out_ref, total = refs[:-2], refs[-2], refs[-1]
    experts = wire_refs[0].shape[0] // 8
    tokens = routes_ref.shape[1]
    features = out_ref.shape[1]
    chosen, rank = ranks(experts, routes_ref)
    weights = (weight_ref[0:1, :], weight_ref[1:2, :])
    total[...] = jnp.zeros_like(total)
    for (parts, _), wire_ref in zip(chunks, wire_refs):
        for part in parts:
            _, _, lane, width = part
            for j in range(features // width):
                found = places(experts, tokens, chosen, rank, part, j)
                scale = jnp.where(found[0], weights[0], 0.0) + jnp.where(found[1], weights[1], 0.0)
                high = scale.astype(bf16)
                low = (scale - high.astype(f32)).astype(bf16)
                held = wire_ref[:, lane : lane + width]
                total[:, j * width : (j + 1) * width] += dot_t(high, held) + dot_t(low, held)
    out_ref[...] = normalize(total[...], gain_ref[...]).astype(out_ref.dtype)


def expert_kernel(parts, count, *refs):
    wires, (gate_ref, up_ref, down_ref) = refs[:count], refs[count : count + 3]
    outs = refs[count + 3 : 2 * count + 3]
    rows_ref, hidden_ref, result_ref = refs[2 * count + 3 :]
    features, hidden = gate_ref.shape
    wide = 512

    places_of = []
    base = 0
    for wire in wires:
        experts = wire.shape[0] // 8
        for size, _, lane, width in parts:
            length = experts * size
            places_of.append((wire, base, length, size, lane, width))
            base += length

    def picking(length, size, j, across):
        shape = (length * 8 // size, length) if across else (length, length * 8 // size)
        row, place = iota(shape, 1 if across else 0), iota(shape, 0 if across else 1)
        return (place == row // size * 8 + j * size + row % size).astype(f32).astype(bf16)

    for wire, start, length, size, lane, width in places_of:
        for j in range(8 // size):
            held = wire[:, lane : lane + width]
            if size < 8:
                held = dot(picking(length, size, j, False), held).astype(bf16)
            rows_ref[start : start + length, j * width : (j + 1) * width] = held

    for start in range(0, hidden, wide):
        cols = slice(start, min(start + wide, hidden))
        gate = dot(rows_ref[...], gate_ref[:, cols])
        up = dot(rows_ref[...], up_ref[:, cols])
        hidden_ref[:, cols] = (gate / (1.0 + jnp.exp(-gate)) * up).astype(bf16)

    def second(i, carry):
        cols = pl.ds(pl.multiple_of(i * wide, wide), wide)
        result_ref[:, cols] = dot(hidden_ref[...], down_ref[:, cols]).astype(bf16)
        return carry

    lax.fori_loop(0, features // wide, second, 0)

    for (wire, start, length, size, lane, width), out in zip(
        places_of, [out for out in outs for _ in parts]
    ):
        total = None
        for j in range(8 // size):
            held = result_ref[start : start + length, j * width : (j + 1) * width]
            if size < 8:
                held = dot(picking(length, size, j, True), held)
            total = held if total is None else total + held
        out[:, lane : lane + width] = total.astype(bf16)


def vmem(count):
    return [pl.BlockSpec(memory_space=pltpu.VMEM)] * count


def expert_block(parts, wires, w_gate, w_up, w_down):
    features, hidden = w_gate.shape
    slots = sum(part[0] for part in parts)
    rows = sum(wire.shape[0] // 8 * slots for wire in wires)
    return pl.pallas_call(
        functools.partial(expert_kernel, parts, len(wires)),
        out_shape=[jax.ShapeDtypeStruct(wire.shape, bf16) for wire in wires],
        in_specs=vmem(len(wires) + 3),
        out_specs=vmem(len(wires)),
        scratch_shapes=[
            pltpu.VMEM((rows, features), bf16),
            pltpu.VMEM((rows, hidden), bf16),
            pltpu.VMEM((rows, features), bf16),
        ],
        compiler_params=pltpu.CompilerParams(vmem_limit_bytes=LIMIT * 2**20),
        cost_estimate=pl.CostEstimate(
            flops=6 * rows * features * hidden,
            bytes_accessed=6 * features * hidden + 4 * rows * features,
            transcendentals=rows * hidden,
        ),
        name="experts",
    )(*wires, w_gate, w_up, w_down)


def ring(step):
    count = lax.axis_size("tp")
    return [(t, (t + step) % count) for t in range(count)]


def rightward(value):
    return lax.ppermute(value, "tp", ring(1))


def leftward(value):
    return lax.ppermute(value, "tp", ring(-1))


def added(*values):
    return sum(value.astype(f32) for value in values).astype(bf16)


def exchange(wire):
    experts = lax.axis_size("ep")
    blocks = wire.reshape(experts, 8, wire.shape[1])
    return lax.all_to_all(blocks, "ep", split_axis=0, concat_axis=0, tiled=True).reshape(wire.shape)


def routed_experts(ffn_in, ffn_gain, routes, route_weight, w_gate, w_up, w_down, out_gain):
    tokens, features = ffn_in.shape
    experts = lax.axis_size("ep")
    chunks = layout(features)
    routes_t, weight_t = routes.T, route_weight.T
    wires = pl.pallas_call(
        functools.partial(pack_kernel, chunks),
        out_shape=[jax.ShapeDtypeStruct((experts * 8, width), bf16) for _, width in chunks],
        in_specs=vmem(3),
        out_specs=vmem(len(chunks)),
        compiler_params=pltpu.CompilerParams(vmem_limit_bytes=8 * 2**20),
        cost_estimate=pl.CostEstimate(flops=2**30, bytes_accessed=2**21, transcendentals=0),
        name="pack",
    )(routes_t, ffn_in, ffn_gain[None])
    ((parts, _),) = chunks
    (wire,) = wires
    compute = functools.partial(expert_block, parts, w_gate=w_gate[0], w_up=w_up[0], w_down=w_down[0])
    own = exchange(wire)
    half = own.shape[0] // 2
    left_a, right_b = rightward(own[:half]), leftward(own[half:])
    left_b, right_a = rightward(own[half:]), leftward(own[:half])
    far_a, far_b = rightward(left_a), leftward(right_b)
    (own,) = compute([own])
    left_a, right_b = compute([left_a, right_b])
    left_b, right_a = compute([left_b, right_a])
    far_a, far_b = compute([far_a, far_b])
    from_right_b, from_left_a = leftward(left_b), rightward(right_a)
    far_a, far_b = leftward(far_a), rightward(far_b)
    from_right_a, from_left_b = leftward(added(left_a, far_a)), rightward(added(right_b, far_b))
    total = jnp.concatenate([added(own[:half], from_left_a, from_right_a), added(own[half:], from_right_b, from_left_b)])
    returned = [exchange(total)]
    return pl.pallas_call(
        functools.partial(combine_kernel, chunks),
        out_shape=jax.ShapeDtypeStruct(ffn_in.shape, bf16),
        in_specs=vmem(3 + len(chunks)),
        out_specs=pl.BlockSpec(memory_space=pltpu.VMEM),
        scratch_shapes=[pltpu.VMEM((tokens, features), f32)],
        compiler_params=pltpu.CompilerParams(vmem_limit_bytes=8 * 2**20),
        cost_estimate=pl.CostEstimate(flops=2**30, bytes_accessed=2**21, transcendentals=0),
        name="combine",
    )(routes_t, weight_t, out_gain[None], *returned)


def pool_mixer(pool_in, pool_map, pool_scale, w_out, mix_gain):
    own_rows, channels = pool_in.shape
    group_count, group_width = pool_map.shape[0], pool_map.shape[1]
    axes = ("ep", "tp")
    count = lax.axis_size(axes)
    previous = lax.ppermute(pool_in[own_rows - 16 :], axes, [(d, d + 1) for d in range(count - 1)])
    running = jnp.concatenate([previous, pool_in], axis=0).astype(f32)
    window_parts = []
    stride = 1
    for step_index in range(group_count):
        running = running[stride:] + running[:-stride]
        stride = stride * 2
        window_parts.append(running[-own_rows:, step_index * group_width : (step_index + 1) * group_width])
    windows = jnp.concatenate(window_parts, axis=1)
    offset = lax.axis_index(axes) * own_rows
    position = (offset + jnp.arange(own_rows, dtype=jnp.int32)).astype(f32)
    reaches = (2 ** (1 + jnp.arange(channels, dtype=jnp.int32) // group_width)).astype(f32)
    counts = jnp.minimum(position[:, None] + 1.0, reaches[None, :])
    contrast = (windows / counts - pool_in.astype(f32)).astype(bf16)
    mapped = jnp.einsum(
        "rgc,gcd->rgd",
        contrast.reshape(own_rows, group_count, group_width),
        pool_map,
        preferred_element_type=f32,
    ).reshape(own_rows, channels)
    pooled = (mapped * pool_scale).astype(bf16)
    projected = jnp.dot(pooled, w_out, preferred_element_type=f32)
    return normalize(projected, mix_gain).astype(bf16)


def shards(
    pool_in,
    pool_map,
    pool_scale,
    w_out,
    mix_gain,
    ffn_in,
    ffn_gain,
    routes,
    route_weight,
    w_gate,
    w_up,
    w_down,
    out_gain,
):
    mixer_out = pool_mixer(pool_in, pool_map, pool_scale, w_out, mix_gain)
    moe_out = routed_experts(ffn_in, ffn_gain, routes, route_weight, w_gate, w_up, w_down, out_gain)
    return (mixer_out, moe_out)


def solution(mesh):
    return jax.shard_map(
        shards,
        mesh=mesh,
        in_specs=(
            P(("ep", "tp"), None),
            P(),
            P(),
            P(),
            P(),
            P(("ep", "tp"), None),
            P(),
            P(("ep", "tp"), None),
            P(("ep", "tp"), None),
            P("ep", None, "tp"),
            P("ep", None, "tp"),
            P("ep", "tp", None),
            P(),
        ),
        out_specs=(P(("ep", "tp"), None), P(("ep", "tp"), None)),
        check_vma=False,
    )
```

```python
import functools

import jax
import jax.numpy as jnp
from jax import lax
from jax.experimental import pallas as pl
from jax.experimental.pallas import tpu as pltpu
from jax.sharding import PartitionSpec as P


epsilon = 1e-06
bf16 = jnp.bfloat16
f32 = jnp.float32

CHUNKS = ((8, 2),)
LIMIT = 14


def layout(features):
    chunks, first = [], 0
    for sizes in CHUNKS:
        parts, lane = [], 0
        for size in sizes:
            parts.append((size, first, lane, size * features // 8))
            first += size
            lane += size * features // 8
        chunks.append((tuple(parts), lane))
    return chunks


def dot(a, b):
    return jnp.dot(a, b, preferred_element_type=f32)


def dot_t(a, b):
    return lax.dot_general(a, b, (((0,), (0,)), ((), ())), preferred_element_type=f32)


def iota(shape, dim):
    return lax.broadcasted_iota(jnp.int32, shape, dim)


def normalize(values, gain):
    return values * lax.rsqrt(jnp.mean(values * values, axis=-1, keepdims=True) + epsilon) * gain


def ranks(experts, routes_ref):
    tokens = routes_ref.shape[1]
    first, second = routes_ref[0:1, :], routes_ref[1:2, :]
    names = iota((experts, tokens), 0)
    hot = [(names == chosen).astype(f32) for chosen in (first, second)]
    before = (iota((tokens, tokens), 0) < iota((tokens, tokens), 1)).astype(bf16)
    ahead = [dot(h.astype(bf16), before) for h in hot]
    ahead[1] = ahead[1] + jnp.sum(hot[0], axis=1, keepdims=True)
    rank = [jnp.sum(h * a, axis=0, keepdims=True).astype(jnp.int32) for h, a in zip(hot, ahead)]
    return (first, second), rank


def places(experts, tokens, chosen, rank, part, j):
    size, first, _, _ = part
    rows = iota((experts * 8, tokens), 0)
    found = []
    for e, r in zip(chosen, rank):
        inside = (r >= first) & (r < first + size)
        found.append(rows == jnp.where(inside, e * 8 + j * size + r - first, -1))
    return found


def pack_kernel(chunks, *refs):
    count = len(chunks)
    sources, wire_refs, buffers, sems = refs[:3], refs[3 : 3 + count], refs[3 + count : 6 + count], refs[6 + count]
    arrivals = [pltpu.make_async_copy(a, b, sems.at[k]) for k, (a, b) in enumerate(zip(sources, buffers))]
    for arrival in arrivals:
        arrival.start()
    routes_ref, rows_ref, gain_ref = buffers
    experts = wire_refs[0].shape[0] // 8
    tokens = routes_ref.shape[1]
    arrivals[0].wait()
    chosen, rank = ranks(experts, routes_ref)
    for arrival in arrivals[1:]:
        arrival.wait()
    normed = normalize(rows_ref[...].astype(f32), gain_ref[...]).astype(bf16)
    for (parts, _), wire_ref in zip(chunks, wire_refs):
        for part in parts:
            _, _, lane, width = part
            total = None
            for j in range(normed.shape[1] // width):
                found = places(experts, tokens, chosen, rank, part, j)
                taken = dot((found[0] | found[1]).astype(f32).astype(bf16), normed[:, j * width : (j + 1) * width])
                total = taken if total is None else total + taken
            wire_ref[:, lane : lane + width] = total.astype(bf16)


def combine_kernel(chunks, routes_ref, weight_ref, gain_ref, *refs):
    wire_refs, out_ref, total = refs[:-2], refs[-2], refs[-1]
    experts = wire_refs[0].shape[0] // 8
    tokens = routes_ref.shape[1]
    features = out_ref.shape[1]
    chosen, rank = ranks(experts, routes_ref)
    weights = (weight_ref[0:1, :], weight_ref[1:2, :])
    total[...] = jnp.zeros_like(total)
    for (parts, _), wire_ref in zip(chunks, wire_refs):
        for part in parts:
            _, _, lane, width = part
            for j in range(features // width):
                found = places(experts, tokens, chosen, rank, part, j)
                scale = jnp.where(found[0], weights[0], 0.0) + jnp.where(found[1], weights[1], 0.0)
                high = scale.astype(bf16)
                low = (scale - high.astype(f32)).astype(bf16)
                held = wire_ref[:, lane : lane + width]
                total[:, j * width : (j + 1) * width] += dot_t(high, held) + dot_t(low, held)
    out_ref[...] = normalize(total[...], gain_ref[...]).astype(out_ref.dtype)


def expert_kernel(parts, count, *refs):
    wires, (gate_ref, up_ref, down_ref) = refs[:count], refs[count : count + 3]
    outs = refs[count + 3 : 2 * count + 3]
    rows_ref, hidden_ref, result_ref = refs[2 * count + 3 :]
    features, hidden = gate_ref.shape
    wide = 512

    places_of = []
    base = 0
    for wire in wires:
        experts = wire.shape[0] // 8
        for size, _, lane, width in parts:
            length = experts * size
            places_of.append((wire, base, length, size, lane, width))
            base += length

    def picking(length, size, j, across):
        shape = (length * 8 // size, length) if across else (length, length * 8 // size)
        row, place = iota(shape, 1 if across else 0), iota(shape, 0 if across else 1)
        return (place == row // size * 8 + j * size + row % size).astype(f32).astype(bf16)

    for wire, start, length, size, lane, width in places_of:
        for j in range(8 // size):
            held = wire[:, lane : lane + width]
            if size < 8:
                held = dot(picking(length, size, j, False), held).astype(bf16)
            rows_ref[start : start + length, j * width : (j + 1) * width] = held

    for start in range(0, hidden, wide):
        cols = slice(start, min(start + wide, hidden))
        gate = dot(rows_ref[...], gate_ref[:, cols])
        up = dot(rows_ref[...], up_ref[:, cols])
        hidden_ref[:, cols] = (gate / (1.0 + jnp.exp(-gate)) * up).astype(bf16)

    def second(i, carry):
        cols = pl.ds(pl.multiple_of(i * wide, wide), wide)
        result_ref[:, cols] = dot(hidden_ref[...], down_ref[:, cols]).astype(bf16)
        return carry

    lax.fori_loop(0, features // wide, second, 0)

    for (wire, start, length, size, lane, width), out in zip(
        places_of, [out for out in outs for _ in parts]
    ):
        total = None
        for j in range(8 // size):
            held = result_ref[start : start + length, j * width : (j + 1) * width]
            if size < 8:
                held = dot(picking(length, size, j, True), held)
            total = held if total is None else total + held
        out[:, lane : lane + width] = total.astype(bf16)


def vmem(count):
    return [pl.BlockSpec(memory_space=pltpu.VMEM)] * count


def expert_block(parts, wires, w_gate, w_up, w_down):
    features, hidden = w_gate.shape
    slots = sum(part[0] for part in parts)
    rows = sum(wire.shape[0] // 8 * slots for wire in wires)
    return pl.pallas_call(
        functools.partial(expert_kernel, parts, len(wires)),
        out_shape=[jax.ShapeDtypeStruct(wire.shape, bf16) for wire in wires],
        in_specs=vmem(len(wires) + 3),
        out_specs=vmem(len(wires)),
        scratch_shapes=[
            pltpu.VMEM((rows, features), bf16),
            pltpu.VMEM((rows, hidden), bf16),
            pltpu.VMEM((rows, features), bf16),
        ],
        compiler_params=pltpu.CompilerParams(vmem_limit_bytes=LIMIT * 2**20),
        cost_estimate=pl.CostEstimate(
            flops=6 * rows * features * hidden,
            bytes_accessed=6 * features * hidden + 4 * rows * features,
            transcendentals=rows * hidden,
        ),
        name="experts",
    )(*wires, w_gate, w_up, w_down)


def ring(step):
    count = lax.axis_size("tp")
    return [(t, (t + step) % count) for t in range(count)]


def rightward(value):
    return lax.ppermute(value, "tp", ring(1))


def leftward(value):
    return lax.ppermute(value, "tp", ring(-1))


def added(*values):
    return sum(value.astype(f32) for value in values).astype(bf16)


def exchange(wire):
    experts = lax.axis_size("ep")
    blocks = wire.reshape(experts, 8, wire.shape[1])
    return lax.all_to_all(blocks, "ep", split_axis=0, concat_axis=0, tiled=True).reshape(wire.shape)


def routed_experts(ffn_in, ffn_gain, routes, route_weight, w_gate, w_up, w_down, out_gain):
    tokens, features = ffn_in.shape
    experts = lax.axis_size("ep")
    chunks = layout(features)
    routes_t, weight_t = routes.T, route_weight.T
    wires = pl.pallas_call(
        functools.partial(pack_kernel, chunks),
        out_shape=[jax.ShapeDtypeStruct((experts * 8, width), bf16) for _, width in chunks],
        in_specs=[pl.BlockSpec(memory_space=pltpu.HBM)] * 3,
        out_specs=vmem(len(chunks)),
        scratch_shapes=[
            pltpu.VMEM(routes_t.shape, routes_t.dtype),
            pltpu.VMEM(ffn_in.shape, ffn_in.dtype),
            pltpu.VMEM((1, features), f32),
            pltpu.SemaphoreType.DMA((3,)),
        ],
        compiler_params=pltpu.CompilerParams(vmem_limit_bytes=60 * 2**20),
        cost_estimate=pl.CostEstimate(flops=2**30, bytes_accessed=2**21, transcendentals=0),
        name="pack",
    )(routes_t, ffn_in, ffn_gain[None])
    ((parts, _),) = chunks
    (wire,) = wires
    compute = functools.partial(expert_block, parts, w_gate=w_gate[0], w_up=w_up[0], w_down=w_down[0])
    own = exchange(wire)
    half = own.shape[0] // 2
    left_a, right_b = rightward(own[:half]), leftward(own[half:])
    left_b, right_a = rightward(own[half:]), leftward(own[:half])
    far_a, far_b = rightward(left_a), leftward(right_b)
    (own,) = compute([own])
    left_a, right_b = compute([left_a, right_b])
    left_b, right_a = compute([left_b, right_a])
    far_a, far_b = compute([far_a, far_b])
    from_right_b, from_left_a = leftward(left_b), rightward(right_a)
    far_a, far_b = leftward(far_a), rightward(far_b)
    from_right_a, from_left_b = leftward(added(left_a, far_a)), rightward(added(right_b, far_b))
    total = jnp.concatenate([added(own[:half], from_left_a, from_right_a), added(own[half:], from_right_b, from_left_b)])
    returned = [exchange(total)]
    return pl.pallas_call(
        functools.partial(combine_kernel, chunks),
        out_shape=jax.ShapeDtypeStruct(ffn_in.shape, bf16),
        in_specs=vmem(3 + len(chunks)),
        out_specs=pl.BlockSpec(memory_space=pltpu.VMEM),
        scratch_shapes=[pltpu.VMEM((tokens, features), f32)],
        compiler_params=pltpu.CompilerParams(vmem_limit_bytes=8 * 2**20),
        cost_estimate=pl.CostEstimate(flops=2**30, bytes_accessed=2**21, transcendentals=0),
        name="combine",
    )(routes_t, weight_t, out_gain[None], *returned)


def pool_mixer(pool_in, pool_map, pool_scale, w_out, mix_gain):
    own_rows, channels = pool_in.shape
    group_count, group_width = pool_map.shape[0], pool_map.shape[1]
    axes = ("ep", "tp")
    count = lax.axis_size(axes)
    previous = lax.ppermute(pool_in[own_rows - 16 :], axes, [(d, d + 1) for d in range(count - 1)])
    running = jnp.concatenate([previous, pool_in], axis=0).astype(f32)
    window_parts = []
    stride = 1
    for step_index in range(group_count):
        running = running[stride:] + running[:-stride]
        stride = stride * 2
        window_parts.append(running[-own_rows:, step_index * group_width : (step_index + 1) * group_width])
    windows = jnp.concatenate(window_parts, axis=1)
    offset = lax.axis_index(axes) * own_rows
    position = (offset + jnp.arange(own_rows, dtype=jnp.int32)).astype(f32)
    reaches = (2 ** (1 + jnp.arange(channels, dtype=jnp.int32) // group_width)).astype(f32)
    counts = jnp.minimum(position[:, None] + 1.0, reaches[None, :])
    contrast = (windows / counts - pool_in.astype(f32)).astype(bf16)
    mapped = jnp.einsum(
        "rgc,gcd->rgd",
        contrast.reshape(own_rows, group_count, group_width),
        pool_map,
        preferred_element_type=f32,
    ).reshape(own_rows, channels)
    pooled = (mapped * pool_scale).astype(bf16)
    projected = jnp.dot(pooled, w_out, preferred_element_type=f32)
    return normalize(projected, mix_gain).astype(bf16)


def shards(
    pool_in,
    pool_map,
    pool_scale,
    w_out,
    mix_gain,
    ffn_in,
    ffn_gain,
    routes,
    route_weight,
    w_gate,
    w_up,
    w_down,
    out_gain,
):
    mixer_out = pool_mixer(pool_in, pool_map, pool_scale, w_out, mix_gain)
    moe_out = routed_experts(ffn_in, ffn_gain, routes, route_weight, w_gate, w_up, w_down, out_gain)
    return (mixer_out, moe_out)


def solution(mesh):
    return jax.shard_map(
        shards,
        mesh=mesh,
        in_specs=(
            P(("ep", "tp"), None),
            P(),
            P(),
            P(),
            P(),
            P(("ep", "tp"), None),
            P(),
            P(("ep", "tp"), None),
            P(("ep", "tp"), None),
            P("ep", None, "tp"),
            P("ep", None, "tp"),
            P("ep", "tp", None),
            P(),
        ),
        out_specs=(P(("ep", "tp"), None), P(("ep", "tp"), None)),
        check_vma=False,
    )
```
